32 devices in a mesh: rep: 2 (over y), fs: 4 (over z), tp: 4 (over x, core).
Axes of the slice: x: 2, y: 2, z: 4, core: 2. Of those that a mesh axis runs over, the one named last changes fastest.
Arguments:
- tokens: bfloat16 [4096, 2048], P(('rep', 'fs'), 'tp'), may hold values from -6 to 6
- outer_gate: float32 [2048, 512], P('fs', 'tp'), may hold values from -0.125 to 0.125
- inner_gate: float32 [2048, 512], P('fs', 'tp'), may hold values from -0.125 to 0.125
- mixer_value: float32 [2048, 512], P('fs', 'tp'), may hold values from -0.125 to 0.125
- mixer_scales: float32 [3, 512], P(None, 'tp'), may hold values from 0.5 to 2
- mixer_taps: float32 [3, 512], P(None, 'tp'), may hold values from -3.5 to 3.5
- mixer_out: float32 [512, 2048], P('fs', 'tp'), may hold values from -0.25 to 0.25
- out_scale: float32 [2048], P('tp'), may hold values from 0.3 to 3
- first_gain: float32 [2048], replicated, may hold values from 0.1 to 1.9
- first_shift: float32 [2048], replicated, may hold values from -2 to 2
- up_proj: float32 [2048, 3072], P('fs', 'tp'), may hold values from -0.125 to 0.125
- gate_proj: float32 [2048, 3072], P('fs', 'tp'), may hold values from -0.125 to 0.125
- up_scales: float32 [2, 3072], P(None, 'tp'), may hold values from 0.5 to 2
- ffn_taps: float32 [3, 2, 3072], P(None, None, 'tp'), may hold values from -3.5 to 3.5
- ffn_shift: float32 [2, 3072], P(None, 'tp'), may hold values from -3 to 3
- down_proj: float32 [3072, 2048], P('fs', 'tp'), may hold values from -0.109375 to 0.109375
- down_scale: float32 [2048], P('tp'), may hold values from 0.3 to 3
- second_gain: float32 [2048], replicated, may hold values from 0.1 to 1.9
- second_shift: float32 [2048], replicated, may hold values from -2 to 2
Outputs:
- layer_out: bfloat16 [4096, 2048], P(('rep', 'fs'), 'tp')
The draws below stay inside these ranges and needn't reach their ends.
All inputs are finite; a program needn't handle non-finite values.
Results may differ from the reference program's by a relative error of at most 0.017.
Values may be sent and summed in bfloat16 or wider, within the bound.
A program may use at most 64 MiB of HBM per device.

```python
import math
import jax
import jax.numpy as jnp
from jax import lax

D = 2048
CW = 512
FF = 3072
LEN = 128
TOKENS = 4096


def shard_levels(rng, shape, split, low, largest):
    def one(position, parts):
        heights = jax.random.uniform(jax.random.fold_in(jax.random.fold_in(rng, 6), position), (parts,), jnp.float32, low / len(split), largest / len(split))
        return jnp.repeat(jnp.exp(heights), shape[position] // parts).reshape((-1,) + (1,) * (len(shape) - position - 1))

    level = one(*split[0])
    for cut in split[1:]:
        level = level * one(*cut)
    return level


def centred(key, dims, width, bound, split=(), kind=jnp.bfloat16):
    array = jax.random.normal(key, dims, jnp.float32) * width
    if len(split) > 0:
        array = shard_levels(key, dims, split, -0.22, 0.18) * array
    return jnp.clip(array, min=-bound, max=bound).astype(kind)


def setup_inputs(seed: int = 0) -> dict:
    key_list = jax.random.split(jax.random.key(seed), 20)
    tokens = centred(key_list[0], (TOKENS, D), 1.0, 6.0, ((0, 8), (1, 4)))
    outer_gate = centred(key_list[1], (D, CW), D ** -0.5, 0.125, ((0, 4), (1, 4)), jnp.float32)
    inner_gate = centred(key_list[2], (D, CW), D ** -0.5, 0.125, ((0, 4), (1, 4)), jnp.float32)
    mixer_value = centred(key_list[3], (D, CW), D ** -0.5, 0.125, ((0, 4), (1, 4)), jnp.float32)
    mixer_scales = jnp.clip(jnp.exp(math.log(2.0) - 1.3862944 * jax.random.uniform(key_list[4], (3, CW), jnp.float32) ** shard_levels(key_list[4], (3, CW), ((1, 4),), -0.2, 0.2)), 0.5, 2.0)
    mixer_taps = centred(key_list[5], (3, CW), 3 ** -0.5, 3.5, ((1, 4),), jnp.float32)
    mixer_out = centred(key_list[6], (CW, D), CW ** -0.5, 0.25, ((0, 4), (1, 4)), jnp.float32)
    out_scale = jnp.clip(jnp.exp(math.log(3.0) - 2.3025851 * jax.random.uniform(key_list[7], (D,), jnp.float32) ** shard_levels(key_list[7], (D,), ((0, 4),), -0.2, 0.2)), 0.3, 3.0)
    first_gain = jnp.clip(1.0 + 0.18 * jax.random.normal(key_list[8], (D,), jnp.float32), 0.1, 1.9)
    first_shift = centred(key_list[9], (D,), 0.3, 2.0, (), jnp.float32)
    up_proj = centred(key_list[10], (D, FF), D ** -0.5, 0.125, ((0, 4), (1, 4)), jnp.float32)
    gate_proj = centred(key_list[11], (D, FF), D ** -0.5, 0.125, ((0, 4), (1, 4)), jnp.float32)
    up_scales = jnp.clip(jnp.exp(math.log(2.0) - 1.3862944 * jax.random.uniform(key_list[12], (2, FF), jnp.float32) ** shard_levels(key_list[12], (2, FF), ((1, 4),), -0.2, 0.2)), 0.5, 2.0)
    ffn_taps = centred(key_list[13], (3, 2, FF), 3 ** -0.5, 3.5, ((2, 4),), jnp.float32)
    ffn_shift = centred(key_list[14], (2, FF), 0.5, 3.0, ((1, 4),), jnp.float32)
    down_proj = centred(key_list[15], (FF, D), FF ** -0.5, 0.109375, ((0, 4), (1, 4)), jnp.float32)
    down_scale = jnp.clip(jnp.exp(math.log(3.0) - 2.3025851 * jax.random.uniform(key_list[16], (D,), jnp.float32) ** shard_levels(key_list[16], (D,), ((0, 4),), -0.2, 0.2)), 0.3, 3.0)
    second_gain = jnp.clip(1.0 + 0.18 * jax.random.normal(key_list[17], (D,), jnp.float32), 0.1, 1.9)
    second_shift = centred(key_list[18], (D,), 0.3, 2.0, (), jnp.float32)
    return {"tokens": tokens, "outer_gate": outer_gate, "inner_gate": inner_gate, "mixer_value": mixer_value, "mixer_scales": mixer_scales, "mixer_taps": mixer_taps, "mixer_out": mixer_out, "out_scale": out_scale, "first_gain": first_gain, "first_shift": first_shift, "up_proj": up_proj, "gate_proj": gate_proj, "up_scales": up_scales, "ffn_taps": ffn_taps, "ffn_shift": ffn_shift, "down_proj": down_proj, "down_scale": down_scale, "second_gain": second_gain, "second_shift": second_shift}


norm_eps = 1e-05
residual_weight = 8.0 ** 0.25

def causal_mix(signal, kernel_taps):
    sequences = signal.reshape(-1, LEN, signal.shape[-1])
    padded = jnp.pad(sequences, ((0, 0), (2, 0), (0, 0)))
    mixed = kernel_taps[0] * padded[:, :-2] + kernel_taps[1] * padded[:, 1:-1] + kernel_taps[2] * padded[:, 2:]
    return mixed.reshape(signal.shape)

def layer_norm(summed, gain_vector, shift_vector):
    average = lax.optimization_barrier(jnp.mean(summed, -1, keepdims=True))
    spread = lax.optimization_barrier(jnp.mean(jnp.square(summed - average), -1, keepdims=True))
    return (summed - average) * lax.rsqrt(spread + norm_eps) * gain_vector + shift_vector

def lowered(matrix):
    return matrix.astype(jnp.bfloat16)

def project(left_rows, matrix, column_scale):
    return jnp.dot(left_rows, lowered(matrix), preferred_element_type=jnp.float32) * column_scale

def reference(tokens, outer_gate, inner_gate, mixer_value, mixer_scales, mixer_taps, mixer_out, out_scale, first_gain, first_shift, up_proj, gate_proj, up_scales, ffn_taps, ffn_shift, down_proj, down_scale, second_gain, second_shift):
    outer_part = project(tokens, outer_gate, mixer_scales[0]).astype(jnp.bfloat16)
    inner_part = project(tokens, inner_gate, mixer_scales[1]).astype(jnp.bfloat16)
    value_part = project(tokens, mixer_value, mixer_scales[2]).astype(jnp.bfloat16)
    product = inner_part.astype(jnp.float32) * value_part.astype(jnp.float32)
    mixed_conv = (outer_part.astype(jnp.float32) * causal_mix(product, mixer_taps)).astype(jnp.bfloat16)
    mixer_sum = project(mixed_conv, mixer_out, out_scale)
    first_sum = residual_weight * tokens.astype(jnp.float32) + mixer_sum
    normed = layer_norm(first_sum, first_gain, first_shift).astype(jnp.bfloat16)
    up_linear = project(normed, up_proj, up_scales[0])
    gate_linear = project(normed, gate_proj, up_scales[1])
    up_mixed = causal_mix(up_linear, ffn_taps[:, 0]) + ffn_shift[0]
    gate_mixed = causal_mix(gate_linear, ffn_taps[:, 1]) + ffn_shift[1]
    hidden = (up_mixed * jax.nn.silu(gate_mixed)).astype(jnp.bfloat16)
    ffn_sum = project(hidden, down_proj, down_scale)
    second_sum = residual_weight * normed.astype(jnp.float32) + ffn_sum
    return layer_norm(second_sum, second_gain, second_shift).astype(jnp.bfloat16)
```

```python
import functools

import jax
import jax.numpy as jnp
from jax import lax
from jax.experimental import pallas as pl
from jax.experimental.pallas import tpu as pltpu
from jax.sharding import PartitionSpec as P

LEN = 128


norm_eps = 1e-05
residual_weight = 8.0**0.25


def causal_mix(signal, kernel_taps):
    sequences = signal.reshape(-1, LEN, signal.shape[-1])
    padded = jnp.pad(sequences, ((0, 0), (2, 0), (0, 0)))
    mixed = (
        kernel_taps[0] * padded[:, :-2]
        + kernel_taps[1] * padded[:, 1:-1]
        + kernel_taps[2] * padded[:, 2:]
    )
    return mixed.reshape(signal.shape)


def lowered(matrix):
    return matrix.astype(jnp.bfloat16)


def single_fold(operand, portion):
    return jnp.dot(operand, portion, preferred_element_type=jnp.float32)


def fold_step(operand, pieces):
    result = []
    for number in range(len(pieces)):
        result.append(jnp.dot(operand, pieces[number], preferred_element_type=jnp.float32))
    return tuple(result)


def own_columns(vector, own_width):
    return lax.dynamic_slice_in_dim(vector, lax.axis_index("tp") * own_width, own_width, 0)


def scaled_norm(summed, average, spread, gain_vector, shift_vector):
    return (summed - average) * lax.rsqrt(spread + norm_eps) * gain_vector + shift_vector


def local(
    tokens,
    outer_gate,
    inner_gate,
    mixer_value,
    mixer_scales,
    mixer_taps,
    mixer_out,
    out_scale,
    first_gain,
    first_shift,
    up_proj,
    gate_proj,
    up_scales,
    ffn_taps,
    ffn_shift,
    down_proj,
    down_scale,
    second_gain,
    second_shift,
):
    own_width = tokens.shape[1]
    full_width = own_width * lax.axis_size("tp")
    token_whole = lax.all_gather(tokens, "tp", axis=1, tiled=True)
    outer_part, inner_part, value_part = fold_step(
        token_whole,
        (
            lax.all_gather(lowered(outer_gate), "fs", axis=0, tiled=True),
            lax.all_gather(lowered(inner_gate), "fs", axis=0, tiled=True),
            lax.all_gather(lowered(mixer_value), "fs", axis=0, tiled=True),
        ),
    )
    outer_part = (outer_part * mixer_scales[0]).astype(jnp.bfloat16)
    inner_part = (inner_part * mixer_scales[1]).astype(jnp.bfloat16)
    value_part = (value_part * mixer_scales[2]).astype(jnp.bfloat16)
    product = inner_part.astype(jnp.float32) * value_part.astype(jnp.float32)
    mixed_conv = (outer_part.astype(jnp.float32) * causal_mix(product, mixer_taps)).astype(
        jnp.bfloat16
    )
    conv_whole = lax.all_gather(mixed_conv, "tp", axis=1, tiled=True)
    mixer_sum = (
        single_fold(conv_whole, lax.all_gather(lowered(mixer_out), "fs", axis=0, tiled=True))
        * out_scale
    )
    first_sum = residual_weight * tokens.astype(jnp.float32) + mixer_sum
    row_total, row_square = lax.psum(
        (jnp.sum(first_sum, 1, keepdims=True), jnp.sum(first_sum * first_sum, 1, keepdims=True)),
        "tp",
    )
    average = row_total / full_width
    spread = row_square / full_width - average * average
    normed = scaled_norm(
        first_sum,
        average,
        spread,
        own_columns(first_gain, own_width),
        own_columns(first_shift, own_width),
    ).astype(jnp.bfloat16)
    normed_whole = lax.all_gather(normed, "tp", axis=1, tiled=True)
    up_matrix, gate_matrix = (
        lax.all_gather(lowered(up_proj), "fs", axis=0, tiled=True),
        lax.all_gather(lowered(gate_proj), "fs", axis=0, tiled=True),
    )
    up_linear = jnp.dot(normed_whole, up_matrix, preferred_element_type=jnp.float32)
    gate_linear = jnp.dot(normed_whole, gate_matrix, preferred_element_type=jnp.float32)
    up_linear = up_linear * up_scales[0]
    gate_linear = gate_linear * up_scales[1]
    up_mixed = causal_mix(up_linear, ffn_taps[:, 0]) + ffn_shift[0]
    gate_mixed = causal_mix(gate_linear, ffn_taps[:, 1]) + ffn_shift[1]
    hidden = (up_mixed * jax.nn.silu(gate_mixed)).astype(jnp.bfloat16)
    hidden_whole = lax.all_gather(hidden, "tp", axis=1, tiled=True)
    ffn_sum = (
        single_fold(hidden_whole, lax.all_gather(lowered(down_proj), "fs", axis=0, tiled=True))
        * down_scale
    )
    second_sum = residual_weight * normed.astype(jnp.float32) + ffn_sum
    second_total, second_square = lax.psum(
        (jnp.sum(second_sum, 1, keepdims=True), jnp.sum(second_sum * second_sum, 1, keepdims=True)),
        "tp",
    )
    second_average = second_total / full_width
    second_spread = second_square / full_width - second_average * second_average
    return scaled_norm(
        second_sum,
        second_average,
        second_spread,
        own_columns(second_gain, own_width),
        own_columns(second_shift, own_width),
    ).astype(jnp.bfloat16)


LANES = 128


def shifted_mix(signal, taps, first_tap):
    rows = lax.broadcasted_iota(jnp.int32, signal.shape, 0) % LEN
    one = jnp.where(rows >= 1, pltpu.roll(signal, 1, 0), 0.0)
    two = jnp.where(rows >= 2, pltpu.roll(signal, 2, 0), 0.0)
    return (
        taps[first_tap : first_tap + 1] * two
        + taps[first_tap + 1 : first_tap + 2] * one
        + taps[first_tap + 2 : first_tap + 3] * signal
    )


def dot32(left, right):
    return jnp.dot(left, right, preferred_element_type=jnp.float32)


def kernel(
    fs,
    tp,
    tokens_hbm,
    outer_hbm,
    inner_hbm,
    value_hbm,
    out_hbm,
    up_hbm,
    gate_hbm,
    down_hbm,
    narrow,
    model,
    wide,
    result,
    mix_f,
    out_f,
    up_f,
    gate_f,
    down_f,
    mix_g,
    out_g,
    ug_g,
    down_g,
    token_all,
    conv_all,
    norm_all,
    hidden_all,
    first_sum,
    total,
    stats,
    load_sem,
    send_z,
    send_y,
    recv_z,
    recv_y,
    send_x,
    recv_x,
    send_s,
    recv_s,
):
    r, z, t = lax.axis_index("rep"), lax.axis_index("fs"), lax.axis_index("tp")
    sibling = t + 1 - 2 * (t % 2)
    across = (t + 2) % tp
    diagonal = (sibling + 2) % tp
    other = 1 - r
    rows, own_width = result.shape
    full_width = own_width * tp
    channels = conv_all.shape[2]
    blocks = ug_g.shape[1]

    sources = (tokens_hbm, outer_hbm, inner_hbm, value_hbm, out_hbm, up_hbm, gate_hbm, down_hbm)
    places = (token_all.at[t], mix_f.at[0], mix_f.at[1], mix_f.at[2], out_f, up_f, gate_f, down_f)
    loads = [
        pltpu.make_async_copy(source, place, load_sem.at[number])
        for number, (source, place) in enumerate(zip(sources, places))
    ]
    for load in loads:
        load.start()

    barrier = pltpu.get_barrier_semaphore()
    for peer in (sibling, across, diagonal):
        pl.semaphore_signal(barrier, inc=1, device_id={"tp": peer}, device_id_type=pl.DeviceIdType.MESH)
    pl.semaphore_signal(barrier, inc=1, device_id={"rep": other}, device_id_type=pl.DeviceIdType.MESH)

    @pl.when(z > 0)
    def _():
        pl.semaphore_signal(barrier, inc=1, device_id={"fs": z - 1}, device_id_type=pl.DeviceIdType.MESH)

    @pl.when(z < fs - 1)
    def _():
        pl.semaphore_signal(barrier, inc=1, device_id={"fs": z + 1}, device_id_type=pl.DeviceIdType.MESH)

    inside = (z > 0) & (z < fs - 1)

    @pl.when(inside)
    def _():
        pl.semaphore_wait(barrier, 6)

    @pl.when(jnp.logical_not(inside))
    def _():
        pl.semaphore_wait(barrier, 5)

    def hop(number, slot, ref, peer, kind):
        return pltpu.make_async_remote_copy(
            src_ref=ref(slot),
            dst_ref=ref(slot),
            send_sem=send_x.at[number, kind],
            recv_sem=recv_x.at[number, slot],
            device_id={"tp": peer},
            device_id_type=pl.DeviceIdType.MESH,
        )

    def exchange_start(number, ref):
        hop(number, t, ref, across, 0).start()
        hop(number, t, ref, sibling, 1).start()

    def exchange_pass(number, ref):
        hop(number, across, ref, across, 0).wait_recv()
        hop(number, across, ref, sibling, 2).start()

    def exchange_end(number, ref):
        hop(number, sibling, ref, sibling, 1).wait_recv()
        hop(number, diagonal, ref, sibling, 2).wait_recv()

    def exchange_sent(number, ref):
        hop(number, t, ref, across, 0).wait_send()
        hop(number, t, ref, sibling, 1).wait_send()
        hop(number, across, ref, sibling, 2).wait_send()

    def token_block(slot):
        return token_all.at[slot]

    def conv_block(slot):
        return conv_all.at[slot]

    def norm_block(slot):
        return norm_all.at[slot]

    def hidden_block(number):
        return lambda slot: hidden_all.at[slot, number]

    def mix_unit(part):
        size = mix_g.shape[1] // 4
        return lambda source, half: mix_g.at[source, pl.ds(pl.multiple_of((part * 2 + half) * size, size), size)]

    def out_unit(source, half):
        size = out_g.shape[1] // 2
        return out_g.at[source, pl.ds(pl.multiple_of(half * size, size), size)]

    def ug_unit(block):
        size = ug_g.shape[2] // 2
        return lambda source, half: ug_g.at[source, block, pl.ds(pl.multiple_of(half * size, size), size)]

    def down_unit(part):
        size = LANES
        return lambda source, half: down_g.at[source, pl.ds(pl.multiple_of((part * 2 + half) * size, size), size)]

    units = [mix_unit(0), mix_unit(1), out_unit]
    units += [ug_unit(block) for block in range(blocks)]
    units += [down_unit(part) for part in range(blocks // 2)]
    count = len(units)
    first_ug, first_down = 3, 3 + blocks

    def along(unit, source, target, way):
        ref = units[unit](source, r)
        return pltpu.make_async_remote_copy(
            src_ref=ref,
            dst_ref=ref,
            send_sem=send_z.at[unit, source, way],
            recv_sem=recv_z.at[unit, source],
            device_id={"fs": target},
            device_id_type=pl.DeviceIdType.MESH,
        )

    def over(unit, source, half):
        ref = units[unit](source, half)
        return pltpu.make_async_remote_copy(
            src_ref=ref,
            dst_ref=ref,
            send_sem=send_y.at[unit, source],
            recv_sem=recv_y.at[unit, source],
            device_id={"rep": other},
            device_id_type=pl.DeviceIdType.MESH,
        )

    def own(unit):
        @pl.when(z < fs - 1)
        def _():
            along(unit, z, z + 1, 0).start()

        @pl.when(z > 0)
        def _():
            along(unit, z, z - 1, 1).start()

    def own_sent(unit):
        @pl.when(z < fs - 1)
        def _():
            along(unit, z, z + 1, 0).wait_send()

        @pl.when(z > 0)
        def _():
            along(unit, z, z - 1, 1).wait_send()

    def passed(unit, distance, sent):
        @pl.when(z >= distance)
        def _():
            source = z - distance
            if not sent:
                along(unit, source, z, 0).wait_recv()

            @pl.when(z < fs - 1)
            def _():
                copy = along(unit, source, z + 1, 0)
                copy.wait_send() if sent else copy.start()

            copy = over(unit, source, r)
            copy.wait_send() if sent else copy.start()

        @pl.when(z + distance < fs)
        def _():
            source = z + distance
            if not sent:
                along(unit, source, z, 1).wait_recv()

            @pl.when(z > 0)
            def _():
                copy = along(unit, source, z - 1, 1)
                copy.wait_send() if sent else copy.start()

            copy = over(unit, source, r)
            copy.wait_send() if sent else copy.start()

    def step(number):
        if number < count:
            own(number)
        for distance in range(1, fs):
            if 0 <= number - distance < count:
                passed(number - distance, distance, False)

    def need(unit):
        for source in range(fs):

            @pl.when(z != source)
            def _():
                over(unit, source, other).wait_recv()

    def lower_block(block):
        columns = slice(block * LANES, (block + 1) * LANES)
        ug_g[z, block, :, :LANES] = up_f[:, columns].astype(jnp.bfloat16)
        ug_g[z, block, :, LANES:] = gate_f[:, columns].astype(jnp.bfloat16)

    def summing(number, peer, slot, kind):
        return pltpu.make_async_remote_copy(
            src_ref=stats.at[number, slot],
            dst_ref=stats.at[number, slot],
            send_sem=send_s.at[number, kind],
            recv_sem=recv_s.at[number, slot],
            device_id={"tp": peer},
            device_id_type=pl.DeviceIdType.MESH,
        )

    def sums_start(number, summed):
        lane = lax.broadcasted_iota(jnp.int32, (rows, LANES), 1)
        one = jnp.sum(summed, axis=1, keepdims=True)
        two = jnp.sum(summed * summed, axis=1, keepdims=True)
        stats[number, t] = jnp.transpose(jnp.where(lane == 0, one, two))[:8]
        for kind, peer in enumerate((across, diagonal, sibling)):
            summing(number, peer, t, kind).start()

    def sums_end(number):
        for kind, peer in enumerate((across, diagonal, sibling)):
            summing(number, peer, peer, kind).wait_recv()
        whole = stats[number, 0]
        for slot in range(1, tp):
            whole = whole + stats[number, slot]
        back = jnp.transpose(jnp.concatenate([whole] * (LANES // 8), axis=0))
        average = back[:, 0:1] / full_width
        return average, back[:, 1:2] / full_width - average * average

    def mixer():
        for unit in (0, 1):
            need(unit)
        exchange_end(0, token_block)
        parts = dot32(token_all[0], mix_g[0])
        for slot in range(1, tp):
            parts = parts + dot32(token_all[slot], mix_g[slot])
        scaled = [
            (parts[:, part * channels : (part + 1) * channels] * narrow[part : part + 1])
            .astype(jnp.bfloat16)
            .astype(jnp.float32)
            for part in range(3)
        ]
        mixed = scaled[0] * shifted_mix(scaled[1] * scaled[2], narrow, 3)
        conv_all[t] = mixed.astype(jnp.bfloat16)
        exchange_start(1, conv_block)

    def mixer_output():
        need(2)
        exchange_end(1, conv_block)
        summed = dot32(conv_all[0], out_g[0])
        for slot in range(1, tp):
            summed = summed + dot32(conv_all[slot], out_g[slot])
        summed = summed * model[0:1] + residual_weight * token_all[t].astype(jnp.float32)
        first_sum[...] = summed
        sums_start(0, summed)

    def first_norm():
        average, spread = sums_end(0)
        norm_all[t] = scaled_norm(first_sum[...], average, spread, model[1:2], model[2:3]).astype(jnp.bfloat16)
        exchange_start(2, norm_block)

    def hidden(block):
        need(first_ug + block)
        both = dot32(norm_all[0], ug_g[0, block])
        for slot in range(1, tp):
            both = both + dot32(norm_all[slot], ug_g[slot, block])
        taps = wide[:, block * LANES : (block + 1) * LANES]
        up_mixed = shifted_mix(both[:, :LANES] * taps[0:1], taps, 2) + taps[8:9]
        gate_mixed = shifted_mix(both[:, LANES:] * taps[1:2], taps, 5) + taps[9:10]
        hidden_all[t, block] = (up_mixed * gate_mixed / (1.0 + jnp.exp(-gate_mixed))).astype(jnp.bfloat16)
        exchange_start(3 + block, hidden_block(block))

    def down(part):
        need(first_down + part)
        for block in (2 * part, 2 * part + 1):
            exchange_end(3 + block, hidden_block(block))
        summed = None
        for slot in range(tp):
            left = jnp.concatenate([hidden_all[slot, 2 * part], hidden_all[slot, 2 * part + 1]], axis=1)
            term = dot32(left, down_g[slot, part * 2 * LANES : (part + 1) * 2 * LANES])
            summed = term if summed is None else summed + term
        total[...] = summed if part == 0 else total[...] + summed

    for load in loads[:4]:
        load.wait()
    exchange_start(0, token_block)
    for part in range(3):
        mix_g[z, :, part * channels : (part + 1) * channels] = mix_f[part].astype(jnp.bfloat16)
    step(0)
    step(1)
    loads[4].wait()
    out_g[z] = out_f[...].astype(jnp.bfloat16)
    step(2)
    exchange_pass(0, token_block)
    loads[5].wait()
    loads[6].wait()
    loads[7].wait()
    lower_block(0)
    step(3)
    lower_block(1)
    step(4)
    mixer()
    lower_block(2)
    step(5)
    exchange_pass(1, conv_block)
    mixer_output()
    lower_block(3)
    step(6)
    first_norm()
    lower_block(4)
    step(7)
    for block in range(5, blocks):
        lower_block(block)
    exchange_pass(2, norm_block)
    step(8)
    down_g[z] = down_f[...].astype(jnp.bfloat16)
    exchange_end(2, norm_block)
    hidden(0)
    number = 9
    ready = 1
    moved = 0
    while ready < blocks:
        step(number)
        number += 1
        while moved < ready:
            exchange_pass(3 + moved, hidden_block(moved))
            moved += 1
        while ready < blocks and first_ug + ready + fs - 1 <= number - 1:
            hidden(ready)
            ready += 1
    for part in range(blocks // 2):
        while number <= first_down + part + fs - 1:
            step(number)
            number += 1
        while moved < blocks:
            exchange_pass(3 + moved, hidden_block(moved))
            moved += 1
        down(part)

    second = total[...] * model[3:4] + residual_weight * norm_all[t].astype(jnp.float32)
    total[...] = second
    sums_start(1, second)

    for unit in range(count):
        own_sent(unit)
        for distance in range(1, fs):
            passed(unit, distance, True)
    refs = [token_block, conv_block, norm_block] + [hidden_block(block) for block in range(blocks)]
    for place, ref in enumerate(refs):
        exchange_sent(place, ref)
    average, spread = sums_end(1)
    result[...] = scaled_norm(total[...], average, spread, model[4:5], model[5:6]).astype(result.dtype)
    for place in range(2):
        for kind, peer in enumerate((across, diagonal, sibling)):
            summing(place, peer, t, kind).wait_send()


def fused(
    fs,
    tp,
    tokens,
    outer_gate,
    inner_gate,
    mixer_value,
    mixer_scales,
    mixer_taps,
    mixer_out,
    out_scale,
    first_gain,
    first_shift,
    up_proj,
    gate_proj,
    up_scales,
    ffn_taps,
    ffn_shift,
    down_proj,
    down_scale,
    second_gain,
    second_shift,
):
    rows, own_width = tokens.shape
    depth, channels = outer_gate.shape
    hidden = up_proj.shape[1]
    blocks = hidden // LANES
    count = 3 + blocks + blocks // 2
    narrow = jnp.concatenate([mixer_scales, mixer_taps], axis=0)
    model = jnp.stack(
        [
            out_scale,
            own_columns(first_gain, own_width),
            own_columns(first_shift, own_width),
            down_scale,
            own_columns(second_gain, own_width),
            own_columns(second_shift, own_width),
        ]
    )
    wide = jnp.concatenate([up_scales, ffn_taps[:, 0], ffn_taps[:, 1], ffn_shift], axis=0)
    any_space = pl.BlockSpec(memory_space=pl.ANY)
    in_vmem = pl.BlockSpec(memory_space=pltpu.VMEM)
    return pl.pallas_call(
        functools.partial(kernel, fs, tp),
        out_shape=jax.ShapeDtypeStruct((rows, own_width), jnp.bfloat16),
        in_specs=[any_space] * 8 + [in_vmem] * 3,
        out_specs=in_vmem,
        scratch_shapes=[
            pltpu.VMEM((3, depth, channels), jnp.float32),
            pltpu.VMEM(mixer_out.shape, jnp.float32),
            pltpu.VMEM(up_proj.shape, jnp.float32),
            pltpu.VMEM(gate_proj.shape, jnp.float32),
            pltpu.VMEM(down_proj.shape, jnp.float32),
            pltpu.VMEM((fs, depth, 3 * channels), jnp.bfloat16),
            pltpu.VMEM((fs,) + mixer_out.shape, jnp.bfloat16),
            pltpu.VMEM((fs, blocks, depth, 2 * LANES), jnp.bfloat16),
            pltpu.VMEM((fs,) + down_proj.shape, jnp.bfloat16),
            pltpu.VMEM((tp, rows, own_width), jnp.bfloat16),
            pltpu.VMEM((tp, rows, channels), jnp.bfloat16),
            pltpu.VMEM((tp, rows, own_width), jnp.bfloat16),
            pltpu.VMEM((tp, blocks, rows, LANES), jnp.bfloat16),
            pltpu.VMEM((rows, own_width), jnp.float32),
            pltpu.VMEM((rows, own_width), jnp.float32),
            pltpu.VMEM((2, tp, 8, rows), jnp.float32),
            pltpu.SemaphoreType.DMA((8,)),
            pltpu.SemaphoreType.DMA((count, fs, 2)),
            pltpu.SemaphoreType.DMA((count, fs)),
            pltpu.SemaphoreType.DMA((count, fs)),
            pltpu.SemaphoreType.DMA((count, fs)),
            pltpu.SemaphoreType.DMA((3 + blocks, 3)),
            pltpu.SemaphoreType.DMA((3 + blocks, tp)),
            pltpu.SemaphoreType.DMA((2, 3)),
            pltpu.SemaphoreType.DMA((2, tp)),
        ],
        compiler_params=pltpu.CompilerParams(
            collective_id=0, has_side_effects=True, vmem_limit_bytes=60 * 1024 * 1024
        ),
    )(
        tokens,
        outer_gate,
        inner_gate,
        mixer_value,
        mixer_out,
        up_proj,
        gate_proj,
        down_proj,
        narrow,
        model,
        wide,
    )


def fits(mesh):
    return mesh.shape["rep"] == 2 and mesh.shape["fs"] == 4 and mesh.shape["tp"] == 4


def solution(mesh):
    body = functools.partial(fused, mesh.shape["fs"], mesh.shape["tp"]) if fits(mesh) else local
    return jax.shard_map(
        body,
        mesh=mesh,
        in_specs=(
            P(("rep", "fs"), "tp"),
            P("fs", "tp"),
            P("fs", "tp"),
            P("fs", "tp"),
            P(None, "tp"),
            P(None, "tp"),
            P("fs", "tp"),
            P("tp"),
            P(),
            P(),
            P("fs", "tp"),
            P("fs", "tp"),
            P(None, "tp"),
            P(None, None, "tp"),
            P(None, "tp"),
            P("fs", "tp"),
            P("tp"),
            P(),
            P(),
        ),
        out_specs=P(("rep", "fs"), "tp"),
        check_vma=False,
    )
```
